1024 devices in a mesh: sp: 128 (over z, y), tp: 8 (over x, core).
Axes of the slice: x: 4, y: 4, z: 32, core: 2. Of those that a mesh axis runs over, the one named last changes fastest.
Arguments:
- latent: bfloat16 [16384, 2048], P(('sp', 'tp')), may hold values from -6 to 6
- context: bfloat16 [512, 2048], replicated, may hold values from -6 to 6
- condition: float32 [2048], replicated, may hold values from -6 to 6
- context_condition: float32 [2048], replicated, may hold values from -6 to 6
- modulation_weight: bfloat16 [2048, 3, 2048], P('sp', None, 'tp'), may hold values from -0.75 to 0.75
- norm_gain: float32 [2048], replicated, may hold values from 0.1 to 1.9
- gate_weight: bfloat16 [2048, 1024], P(None, 'tp'), may hold values from -0.125 to 0.125
- value_weight: bfloat16 [2048, 1024], P(None, 'tp'), may hold values from -0.125 to 0.125
- write_weight: bfloat16 [2048, 512], P(None, 'tp'), may hold values from -0.125 to 0.125
- read_weight: bfloat16 [2048, 512], P(None, 'tp'), may hold values from -0.125 to 0.125
- step_weight: bfloat16 [2048, 2, 16], replicated, may hold values from -0.125 to 0.125
- value_taps: bfloat16 [3, 1024], P(None, 'tp'), may hold values from -3.5 to 3.5
- map_taps: bfloat16 [3, 2, 512], P(None, None, 'tp'), may hold values from -3.5 to 3.5
- decay_rate: float32 [2, 16], replicated, may hold values from 1e-06 to 0.06
- decay_jump: float32 [2, 16, 16384], P(None, 'tp', 'sp'), may hold values from -2.76 to 0
- skip_gain: float32 [16], replicated, may hold values from 1 to 16
- group_gain: float32 [1024], P('tp'), may hold values from 0.1 to 1.9
- output_weight: bfloat16 [1024, 2048], P('tp'), may hold values from -0.1875 to 0.1875
- post_gain: float32 [2048], replicated, may hold values from 0.1 to 1.9
Outputs:
- updated: bfloat16 [16384, 2048], P(('sp', 'tp'))
The draws below stay inside these ranges and needn't reach their ends.
All inputs are finite; a program needn't handle non-finite values.
Results may differ from the reference program's by a relative error of at most 0.014.
Values may be sent and summed in bfloat16 or wider, within the bound.
A program may use at most 64 MiB of HBM per device.

```python
import math
import jax
import jax.numpy as jnp
from jax import lax

D = 2048
HEADS = 16
HEAD_DIM = 64
GROUPS = 8
STATE = 64
SPAN = 128
CTX = 512
INNER = 1024
TOKENS = 16384
N_TP = 8


def draw_decay_rate(key, part):
    pick_key, value_key = jax.random.split(jax.random.fold_in(key, 11))
    fast_heads = jax.random.randint(pick_key, (2, HEADS), 0, 2) == 1
    spread = jax.random.uniform(value_key, (2, HEADS), jnp.float32)
    slow_rate = jnp.exp(jnp.log(1e-06) + spread * (jnp.log(6e-05) - jnp.log(1e-06)))
    fast_rate = jnp.exp(jnp.log(0.02) + spread * (jnp.log(0.06) - jnp.log(0.02)))
    return jnp.where(fast_heads, fast_rate, slow_rate)


def draw_decay_jump(key, part):
    place_key, depth_key = jax.random.split(jax.random.fold_in(key, 23))
    places = jax.random.randint(place_key, (2, HEADS, 4), 0, TOKENS)
    depths = jax.random.uniform(depth_key, (2, HEADS, 4), jnp.float32, 0.22, 0.69)
    positions = jnp.arange(TOKENS, dtype=jnp.int32)
    hits = (positions[None, None, None, :] == places[..., None]).astype(jnp.float32)
    return -jnp.sum(hits * depths[..., None], axis=2)


def strengthened(result, key, source, target, parts, factor):
    def block_of(axis_at):
        return (jnp.arange(result.shape[axis_at]) // (result.shape[axis_at] // parts)).reshape((-1,) + (1,) * (result.ndim - 1 - axis_at))

    one_side = jax.random.permutation(key, parts)[block_of(target)]
    far = (block_of(target) + parts // 2) % parts
    return jnp.where((block_of(source) == one_side) | (block_of(source) == far), factor * result, result)


def level_of(own_key, extent, cuts, smallest, top_value):
    factor_of, own = 1.0, jax.random.fold_in(own_key, 6)
    for position, shards_of in cuts:
        heights = jnp.exp(jax.random.uniform(jax.random.fold_in(own, position), (shards_of,), jnp.float32, smallest / len(cuts), top_value / len(cuts)))
        factor_of = factor_of * jnp.repeat(heights, extent[position] // shards_of).reshape([-1 if axis == position else 1 for axis in range(len(extent))])
    return factor_of


def scatter_about(own_key, shape, scale, limit, pieces=(), kind=jnp.bfloat16):
    entries = scale * jax.random.normal(own_key, shape, jnp.float32)
    if pieces:
        entries = entries * level_of(own_key, shape, pieces, -0.22, 0.18)
    return jnp.clip(entries, -limit, limit).astype(kind)


def gaussian_with(stream_key, dims, scale, limit, cuts, heavy, held_as=jnp.bfloat16):
    drawn = scale * jax.random.normal(stream_key, dims, jnp.float32)
    if cuts:
        drawn = drawn * level_of(stream_key, dims, cuts, -0.22, 0.18)
    return jnp.clip(strengthened(drawn, jax.random.fold_in(stream_key, 3), *heavy), -limit, limit).astype(held_as)


def setup_inputs(seed: int = 0) -> dict:
    streams_of = jax.random.split(jax.random.key(seed), 20)
    latent = scatter_about(streams_of[0], (TOKENS, D), 1.0, 6.0, ((0, 1024),))
    context = scatter_about(streams_of[1], (CTX, D), 1.0, 6.0)
    condition = scatter_about(streams_of[2], (D,), 1.0, 6.0, (), jnp.float32)
    context_condition = scatter_about(streams_of[3], (D,), 1.0, 6.0, (), jnp.float32)
    modulation_weight = gaussian_with(streams_of[4], (D, 3, D), (D // 2) ** -0.5, 0.75, ((0, 128), (2, 8)), (0, 2, 128, 5.5))
    norm_gain = jnp.clip(1.0 + 0.18 * jax.random.normal(streams_of[5], (D,), jnp.float32), 0.1, 1.9)
    gate_weight = scatter_about(streams_of[6], (D, INNER), D ** -0.5, 0.125, ((1, 8),))
    value_weight = scatter_about(streams_of[7], (D, INNER), D ** -0.5, 0.125, ((1, 8),))
    write_weight = scatter_about(streams_of[8], (D, GROUPS * STATE), D ** -0.5, 0.125, ((1, 8),))
    read_weight = scatter_about(streams_of[9], (D, GROUPS * STATE), D ** -0.5, 0.125, ((1, 8),))
    step_weight = scatter_about(streams_of[10], (D, 2, HEADS), D ** -0.5, 0.125)
    value_taps = scatter_about(streams_of[11], (3, INNER), 3 ** -0.5, 3.5, ((1, 8),))
    map_taps = scatter_about(streams_of[12], (3, 2, GROUPS * STATE), 3 ** -0.5, 3.5, ((2, 8),))
    decay_rate = draw_decay_rate(jax.random.fold_in(streams_of[19], 71), 0)
    decay_jump = draw_decay_jump(jax.random.fold_in(streams_of[19], 71), 0)
    skip_gain = jnp.clip(jnp.exp(jax.random.uniform(streams_of[15], (HEADS,), jnp.float32, math.log(1.0), math.log(16.0))), 1.0, 16.0)
    group_gain = jnp.clip(1.0 + 0.18 * jax.random.normal(streams_of[16], (INNER,), jnp.float32), 0.1, 1.9)
    output_weight = scatter_about(streams_of[17], (INNER, D), INNER ** -0.5, 0.1875, ((0, 8),))
    post_gain = jnp.clip(1.0 + 0.18 * jax.random.normal(streams_of[18], (D,), jnp.float32), 0.1, 1.9)
    return dict(latent=latent, context=context, condition=condition, context_condition=context_condition, modulation_weight=modulation_weight, norm_gain=norm_gain, gate_weight=gate_weight, value_weight=value_weight, write_weight=write_weight, read_weight=read_weight, step_weight=step_weight, value_taps=value_taps, map_taps=map_taps, decay_rate=decay_rate, decay_jump=decay_jump, skip_gain=skip_gain, group_gain=group_gain, output_weight=output_weight, post_gain=post_gain)


EPSILON = 1e-06
HIGHEST = lax.Precision.HIGHEST

def modulated_norm(row_block, gain_vec, shift_vec, scale_vec):
    widened = row_block.astype(jnp.float32)
    normed = widened * lax.rsqrt(lax.optimization_barrier(jnp.mean(widened * widened, axis=-1, keepdims=True)) + EPSILON)
    return (normed * gain_vec * (1.0 + scale_vec) + shift_vec).astype(jnp.bfloat16)

def short_conv(padded, conv_taps):
    length = padded.shape[0] - 2
    widened = padded.astype(jnp.float32)
    weights = conv_taps.astype(jnp.float32)
    summed = weights[0] * widened[:length] + weights[1] * widened[1:length + 1] + weights[2] * widened[2:]
    return jax.nn.silu(summed)

def zero_rim(tensor):
    return jnp.pad(tensor, ((1, 1), (0, 0)))

def project(row_block, weight):
    return jnp.dot(row_block, weight, preferred_element_type=jnp.float32).astype(jnp.bfloat16)

def flip_rows(tensor, direction):
    if direction == 1:
        return jnp.flip(tensor, axis=0)
    return tensor

def sweep(inputs, step_sizes, log_decay, write_maps, read_maps, start_state):
    length, head_count, head_width = inputs.shape
    blocks = length // SPAN
    lower_mask = (jnp.arange(SPAN)[:, None] >= jnp.arange(SPAN)[None, :])[:, :, None]

    def cut_blocks(tensor):
        return tensor.reshape((blocks, SPAN) + tensor.shape[1:])

    def advance(carry_state, block_data):
        value_block, size_block, decay_block, write_block, read_block = block_data
        within = jnp.cumsum(decay_block, axis=0)
        weighted = value_block * size_block[:, :, None]
        log_gaps = jnp.where(lower_mask, within[:, None, :] - within[None, :, :], 0.0)
        fading = jnp.where(lower_mask, jnp.exp(log_gaps), 0.0)
        scores = jnp.einsum('ihn,jhn->ijh', read_block, write_block, precision=HIGHEST) * fading
        inner_term = jnp.einsum('ijh,jhp->ihp', scores, weighted, precision=HIGHEST)
        carried = jnp.einsum('ihn,hpn->ihp', read_block * jnp.exp(within)[:, :, None], carry_state, precision=HIGHEST)
        block_total = within[-1]
        fresh_state = jnp.einsum('jhn,jhp->hpn', write_block * jnp.exp(block_total[None, :] - within)[:, :, None], weighted, precision=HIGHEST)
        return (jnp.exp(block_total)[:, None, None] * carry_state + fresh_state, inner_term + carried)
    final_state, outputs = lax.scan(advance, start_state, (cut_blocks(inputs), cut_blocks(step_sizes), cut_blocks(log_decay), cut_blocks(write_maps), cut_blocks(read_maps)))
    return (outputs.reshape(length, head_count, head_width), final_state)

def reference(latent, context, condition, context_condition, modulation_weight, norm_gain, gate_weight, value_weight, write_weight, read_weight, step_weight, value_taps, map_taps, decay_rate, decay_jump, skip_gain, group_gain, output_weight, post_gain):
    conditions = jax.nn.silu(jnp.stack([condition, context_condition]))
    modulation = jnp.einsum('sd,dkc->skc', conditions, modulation_weight.astype(jnp.float32), precision=HIGHEST)
    hidden = modulated_norm(latent, norm_gain, modulation[0, 0], modulation[0, 1])
    context_hidden = modulated_norm(context, norm_gain, modulation[1, 0], modulation[1, 1])
    step_matrix = step_weight.reshape(D, 2 * HEADS)
    gate_linear = project(hidden, gate_weight)
    step_linear = project(hidden, step_matrix).reshape(TOKENS, 2, HEADS)
    repeat_count = HEADS // GROUPS
    latent_values = short_conv(zero_rim(project(hidden, value_weight)), value_taps).reshape(TOKENS, HEADS, HEAD_DIM)
    latent_write = short_conv(zero_rim(project(hidden, write_weight)), map_taps[:, 0]).reshape(TOKENS, GROUPS, STATE)
    latent_read = short_conv(zero_rim(project(hidden, read_weight)), map_taps[:, 1]).reshape(TOKENS, GROUPS, STATE)
    latent_write = jnp.repeat(latent_write, repeat_count, axis=1)
    latent_read = jnp.repeat(latent_read, repeat_count, axis=1)
    context_values = short_conv(zero_rim(project(context_hidden, value_weight)), value_taps).reshape(CTX, HEADS, HEAD_DIM)
    context_write = short_conv(zero_rim(project(context_hidden, write_weight)), map_taps[:, 0]).reshape(CTX, GROUPS, STATE)
    context_write = jnp.repeat(context_write, repeat_count, axis=1)
    context_step = project(context_hidden, step_matrix).reshape(CTX, 2, HEADS)
    mixer_sum = skip_gain[None, :, None] * latent_values
    zero_state = jnp.zeros((HEADS, HEAD_DIM, STATE), jnp.float32)
    for direction in range(2):
        rate_head = decay_rate[direction]
        latent_size = jax.nn.softplus(step_linear[:, direction].astype(jnp.float32))
        latent_decay = -latent_size * rate_head[None, :] + decay_jump[direction].T
        context_size = jax.nn.softplus(context_step[:, direction].astype(jnp.float32))
        context_decay = -context_size * rate_head[None, :]
        unused_rows, context_state = sweep(flip_rows(context_values, direction), flip_rows(context_size, direction), flip_rows(context_decay, direction), flip_rows(context_write, direction), flip_rows(context_write, direction), zero_state)
        swept_rows, unused_state = sweep(flip_rows(latent_values, direction), flip_rows(latent_size, direction), flip_rows(latent_decay, direction), flip_rows(latent_write, direction), flip_rows(latent_read, direction), context_state)
        mixer_sum = mixer_sum + flip_rows(swept_rows, direction)
    gated_rows = mixer_sum.reshape(TOKENS, INNER) * jax.nn.silu(gate_linear.astype(jnp.float32))
    grouped = gated_rows.reshape(TOKENS, GROUPS, INNER // GROUPS)
    grouped = grouped * lax.rsqrt(lax.optimization_barrier(jnp.mean(grouped * grouped, axis=-1, keepdims=True)) + EPSILON) * group_gain.reshape(GROUPS, INNER // GROUPS)
    gated_rows = grouped.reshape(TOKENS, INNER).astype(jnp.bfloat16)
    share = INNER // N_TP
    mixed_rows = jnp.zeros((TOKENS, D), jnp.float32)
    for piece in range(N_TP):
        partial_value = jnp.dot(gated_rows[:, piece * share:(piece + 1) * share], output_weight[piece * share:(piece + 1) * share], preferred_element_type=jnp.float32)
        mixed_rows = mixed_rows + lax.optimization_barrier(partial_value.astype(jnp.bfloat16)).astype(jnp.float32)
    normed_out = mixed_rows * lax.rsqrt(lax.optimization_barrier(jnp.mean(mixed_rows * mixed_rows, axis=-1, keepdims=True)) + EPSILON) * post_gain
    return (latent.astype(jnp.float32) + modulation[0, 2] * normed_out).astype(jnp.bfloat16)
```

```python
import jax
import jax.numpy as jnp
from jax import lax
from jax.experimental import pallas as pl
from jax.experimental.pallas import tpu as pltpu
from jax.sharding import Mesh
from jax.sharding import PartitionSpec as P

SP = ("za", "zb", "y")
SP_TP = ("za", "zb", "y", "tp")
MESH = pl.DeviceIdType.MESH
EPSILON = 1e-06
HIGHEST = lax.Precision.HIGHEST
F32 = jnp.float32
BF16 = jnp.bfloat16
NA, NB, NY, NT = 8, 4, 4, 8
NI = NB * NY
NS = NA * NI
D = 2048
ROWS = 16
RANGE = 128
CTX = 512


def silu(x):
    return x * (1.0 / (1.0 + jnp.exp(-x)))


def softplus(x):
    return jnp.maximum(x, 0.0) + jnp.log1p(jnp.exp(-jnp.abs(x)))


def dot_f32(x, y):
    return jnp.dot(x, y, precision=HIGHEST, preferred_element_type=F32)


def dot_bf16(x, y):
    return jnp.dot(x.astype(BF16), y.astype(BF16), preferred_element_type=F32)


def iota(shape, dim):
    return lax.broadcasted_iota(jnp.int32, shape, dim)


def kernel(
    latent,
    cond,
    ccond,
    modw,
    ngain,
    vtaps,
    mtaps,
    rate,
    jump,
    skip,
    ggain,
    pgain,
    context_h,
    gate_h,
    value_h,
    write_h,
    read_h,
    step_h,
    outw_h,
    out,
    context_v,
    write_v,
    read_v,
    step_v,
    outw_v,
    wall,
    part,
    r1,
    s1,
    r2,
    r3,
    r4,
    xg,
    xn,
    cn,
    hid,
    hctx,
    uctx,
    lsend,
    rl1,
    l2send,
    rl2,
    sp,
    rs1,
    bt,
    rs2,
    cpre,
    ppre,
    cst,
    osend,
    rs3,
    oo,
    ro,
    load_sem,
    near_ssem,
    near_rsem,
    far_ssem,
    far_rsem,
    tp_ssem,
    tp_rsem,
    y_ssem,
    y_rsem,
    halo_ssem,
    halo_rsem,
):
    a = lax.axis_index("za")
    b = lax.axis_index("zb")
    y = lax.axis_index("y")
    t = lax.axis_index("tp")
    i = b * NY + y
    s = a * NI + i
    direction = lax.div(i, 8)

    def near(j):
        return {"zb": lax.div(j, NY), "y": lax.rem(j, NY)}

    def far(j):
        return {"za": j}

    def along_y(j):
        return {"y": j}

    def along_tp(j):
        return {"tp": j}

    def at_range(n):
        return {"za": lax.div(n, NI), "zb": lax.div(lax.rem(n, NI), NY), "y": lax.rem(n, NY)}

    following = at_range(lax.rem(s + 1, NS))
    preceding = at_range(lax.rem(s + NS - 1, NS))

    def copy(src, dst, ssem, rsem, device):
        return pltpu.make_async_remote_copy(
            src_ref=src, dst_ref=dst, send_sem=ssem, recv_sem=rsem, device_id=device, device_id_type=MESH
        )

    def exchange(n, me, peer, src_of, dst, ssem, rsem):
        def begin(k, carry):
            j = lax.rem(me + k, n)
            copy(src_of(j), dst.at[me], ssem.at[k], rsem.at[me], peer(j)).start()
            return carry

        def arrive(k, carry):
            j = lax.rem(me + n - k, n)
            copy(src_of(j), dst.at[j], ssem.at[k], rsem.at[j], peer(j)).wait_recv()
            return carry

        def leave(k, carry):
            j = lax.rem(me + k, n)
            copy(src_of(j), dst.at[me], ssem.at[k], rsem.at[me], peer(j)).wait_send()
            return carry

        return (
            lambda: lax.fori_loop(1, n, begin, 0),
            lambda: lax.fori_loop(1, n, arrive, 0),
            lambda: lax.fori_loop(1, n, leave, 0),
        )

    barrier = pltpu.get_barrier_semaphore()

    def tell(device):
        pl.semaphore_signal(barrier, inc=1, device_id=device, device_id_type=MESH)

    def tell_all(n, me, peer):
        def one(k, carry):
            tell(peer(lax.rem(me + k, n)))
            return carry

        lax.fori_loop(1, n, one, 0)

    tell_all(NA, a, far)
    tell_all(NI, i, near)
    tell_all(NT, t, along_tp)
    tell(following)
    tell(preceding)

    loads = [
        pltpu.make_async_copy(gate_h, wall.at[:, pl.ds(0, 128)], load_sem.at[0]),
        pltpu.make_async_copy(value_h, wall.at[:, pl.ds(128, 128)], load_sem.at[1]),
        pltpu.make_async_copy(write_h, write_v, load_sem.at[2]),
        pltpu.make_async_copy(read_h, read_v, load_sem.at[3]),
        pltpu.make_async_copy(step_h, step_v, load_sem.at[4]),
        pltpu.make_async_copy(context_h, context_v, load_sem.at[5]),
        pltpu.make_async_copy(outw_h, outw_v, load_sem.at[6]),
    ]
    for load in loads:
        load.start()

    lane = iota((1, 128), 1)
    mine = lax.div(lane, ROWS) == lax.rem(s, 8)
    rows8 = iota((8, 128), 0)
    first = jnp.where(mine, silu(cond[pl.ds(lax.div(s, 8), 1), :]), 0.0)
    second = jnp.where(mine, silu(ccond[pl.ds(lax.div(s, 8), 1), :]), 0.0)
    both = jnp.where(rows8 == 0, first, jnp.where(rows8 == 1, second, 0.0))
    weight = modw[...].astype(F32)
    pieces = dot_f32(both, jnp.concatenate([weight] * 8, axis=0))
    for m in range(12):
        r, k, half = m // 6, (m % 6) // 2, m % 2
        low = k * 256 + half * 128
        part[m // 3, m % 3 : m % 3 + 1, :] = pieces[r : r + 1, low : low + 128]

    m1_start, m1_wait, m1_left = exchange(
        NI, i, near, lambda j: part.at[lax.rem(j, NY)], r1, near_ssem.at[0], near_rsem.at[0]
    )
    m2_start, m2_wait, m2_left = exchange(NA, a, far, lambda j: s1, r2, far_ssem.at[0], far_rsem.at[0])
    m3_start, m3_wait, m3_left = exchange(NY, y, along_y, lambda j: r3.at[y], r3, y_ssem, y_rsem)
    m4_start, m4_wait, m4_left = exchange(NT, t, along_tp, lambda j: r3, r4, tp_ssem.at[1], tp_rsem.at[1])
    x_start, x_wait, x_left = exchange(NT, t, along_tp, lambda j: latent, xg, tp_ssem.at[0], tp_rsem.at[0])

    pl.semaphore_wait(barrier, (NA - 1) + (NI - 1) + (NT - 1) + 2)

    m1_start()
    r1[i] = part[y]
    x_start()
    xg[t] = latent[...]

    for load in loads[:5]:
        load.wait()

    def join(k, carry):
        at = pl.ds(pl.multiple_of(k * 256, 256), 256)
        wall[at, 256:384] = jnp.concatenate([write_v[at, :], read_v[at, :]], axis=1)
        wall[at, 384:512] = jnp.concatenate([step_v[at, :], jnp.zeros((256, 96), BF16)], axis=1)
        return carry

    lax.fori_loop(0, D // 256, join, 0)

    m1_wait()
    s1[...] = jnp.sum(r1[...], axis=0)
    m2_start()
    r2[a] = s1[...]

    x_wait()
    up = copy(xg.at[NT - 1], xg.at[NT], halo_ssem.at[0], halo_rsem.at[0], following)
    down = copy(xg.at[0], xg.at[NT + 1], halo_ssem.at[1], halo_rsem.at[1], preceding)
    up.start()
    down.start()
    gain = ngain[...]

    def normed(x):
        return x * lax.rsqrt(jnp.mean(x * x, axis=-1, keepdims=True) + EPSILON) * gain

    def norm_latent(k, carry):
        xn[k] = normed(xg[k].astype(F32))
        return carry

    lax.fori_loop(0, NT, norm_latent, 0)
    up.wait_recv()
    down.wait_recv()
    lax.fori_loop(NT, NT + 2, norm_latent, 0)
    loads[5].wait()

    def norm_context(k, carry):
        at = pl.ds(pl.multiple_of(k * 16, 16), 16)
        cn[at, :] = normed(context_v[at, :].astype(F32))
        return carry

    lax.fori_loop(0, CTX // 16, norm_context, 0)

    m2_wait()
    r3[y] = jnp.sum(r2[...], axis=0)
    m3_start()
    m3_wait()
    m4_start()
    r4[t] = r3[...]
    m4_wait()

    def vector(r, k):
        found = []
        for j in range(NT):
            for half in range(2):
                m = (r * 3 + k) * 2 + half
                found.append(r4[j, m // 3, m % 3 : m % 3 + 1, :])
        return jnp.concatenate(found, axis=1)

    shift0, scale0 = vector(0, 0), 1.0 + vector(0, 1)

    def modulate(k, carry):
        hid[pl.ds(pl.multiple_of(k * 16, 16), 16), :] = (xn[k] * scale0 + shift0).astype(BF16)
        return carry

    lax.fori_loop(0, NT + 2, modulate, 0)
    linear = jnp.dot(hid[...], wall[...], preferred_element_type=F32).astype(BF16).astype(F32)
    gate_linear = linear[:RANGE, :128]
    u = linear[:RANGE, 128:384]
    step_linear = linear[:RANGE, 384:512]
    before = jnp.where(s > 0, linear[RANGE + 15 : RANGE + 16, 128:384], 0.0)
    after = jnp.where(s < NS - 1, linear[RANGE + 16 : RANGE + 17, 128:384], 0.0)
    vt = vtaps[...].astype(F32)

    def taps(k):
        m = mtaps[k].astype(F32)
        return jnp.concatenate([vt[k : k + 1, :], m[0:1, :], m[1:2, :]], axis=1)

    tap = [taps(k) for k in range(3)]

    def conv(u, before, after):
        n = u.shape[0]
        row = iota(u.shape, 0)
        lower = jnp.where(row == 0, before, pltpu.roll(u, 1, 0))
        upper = jnp.where(row == n - 1, after, pltpu.roll(u, n - 1, 0))
        return silu(tap[0] * lower + tap[1] * u + tap[2] * upper)

    k8 = iota((8, 128), 0)
    lane8 = iota((8, 128), 1)
    chosen = jnp.where((k8 < 4) & (lane8 == lax.div(k8, 2) * 16 + 2 * t + lax.rem(k8, 2)), 1.0, 0.0)

    def own_steps(step_linear):
        return softplus(
            lax.dot_general(
                chosen.astype(BF16),
                step_linear.astype(BF16),
                (((1,), (1,)), ((), ())),
                preferred_element_type=F32,
            )
        )

    rates = jnp.zeros((8, 128), F32)
    for k in range(4):
        rates = jnp.where(k8 == k, rate[k // 2, 2 * t + k % 2], rates)
    jumps = jnp.concatenate([jump[0], jump[1], jnp.zeros((4, 128), F32)], axis=0)
    size_row = own_steps(step_linear)
    decay_row = jumps - size_row * rates
    ri = iota((128, 128), 0)
    ci = iota((128, 128), 1)
    upto = jnp.where(ri <= ci, 1.0, 0.0)
    onwards = jnp.where(ri >= ci, 1.0, 0.0)
    within_row = jnp.where(k8 < 2, dot_f32(decay_row, upto), dot_f32(decay_row, onwards))
    total = jnp.sum(decay_row, axis=1, keepdims=True)
    low_lanes = lane < 64

    def total_lanes(d):
        return jnp.where(low_lanes, total[2 * d : 2 * d + 1, :], total[2 * d + 1 : 2 * d + 2, :])

    lsend[0:1, :] = total_lanes(0)
    lsend[1:2, :] = total_lanes(1)
    l1_start, l1_wait, l1_left = exchange(NI, i, near, lambda j: lsend, rl1, near_ssem.at[1], near_rsem.at[1])
    l1_start()
    rl1[i] = lsend[...]

    columns = jnp.concatenate(
        [within_row, jnp.exp(total - within_row) * size_row, jnp.exp(within_row), jnp.zeros((104, 128), F32)],
        axis=0,
    ).T

    def head_columns(columns, base, d):
        at = base + 2 * d
        return jnp.where(low_lanes, columns[:, at : at + 1], columns[:, at + 1 : at + 2])

    mixed = conv(u, before, after)
    values = mixed[:, :128]
    writes = mixed[:, 128:192].astype(BF16)
    reads = mixed[:, 192:256].astype(BF16)

    def state_of(writes, weighted):
        return lax.dot_general(
            writes.astype(BF16),
            weighted.astype(BF16),
            (((0,), (0,)), ((), ())),
            preferred_element_type=F32,
        )

    for d in range(2):
        sp[8 * d : 8 * d + 8] = state_of(writes, values * head_columns(columns, 8, d)).reshape(8, 8, 128)
    s1_start, s1_wait, s1_left = exchange(NI, i, near, lambda j: sp.at[j], rs1, near_ssem.at[2], near_rsem.at[2])
    s1_start()
    rs1[i] = sp[i]

    scores = lax.dot_general(reads, writes, (((1,), (1,)), ((), ())), preferred_element_type=F32)
    inner = []
    for h in range(2):
        fading = jnp.zeros((128, 128), F32)
        for d in range(2):
            k = 2 * d + h
            gap = columns[:, k : k + 1] - within_row[k : k + 1, :]
            mask = (ri >= ci) if d == 0 else (ri <= ci)
            fading = fading + jnp.exp(jnp.where(mask, gap, -1e30)) * size_row[k : k + 1, :]
        inner.append(dot_bf16(scores * fading, values[:, 64 * h : 64 * h + 64]))
    skips = jnp.where(low_lanes, skip[2 * t], skip[2 * t + 1])
    local = skips * values + jnp.concatenate(inner, axis=1)
    gates = silu(gate_linear)

    l1_wait()
    l2send[...] = jnp.sum(rl1[...], axis=0)
    l2_start, l2_wait, l2_left = exchange(NA, a, far, lambda j: l2send, rl2, far_ssem.at[1], far_rsem.at[1])
    l2_start()
    rl2[a] = l2send[...]

    s1_wait()

    def fold(k, carry):
        state, product = carry
        j = k + direction * (NI - 1 - 2 * k)
        cpre[j] = state
        ppre[j] = product
        logs = rl1[j]
        factor = jnp.exp(jnp.where(direction == 0, logs[0:1, :], logs[1:2, :]))
        return factor * state + rs1[j], factor * product

    block_state, _ = lax.fori_loop(
        0, NI, fold, (jnp.zeros((8, 128), F32), jnp.ones((1, 128), F32))
    )
    bt[...] = block_state
    s2_start, s2_wait, s2_left = exchange(NA, a, far, lambda j: bt, rs2, far_ssem.at[2], far_rsem.at[2])
    s2_start()
    rs2[a] = bt[...]

    shift1, scale1 = vector(1, 0), 1.0 + vector(1, 1)

    def context_chunk(k, carry):
        def mod(m, carry):
            at = pl.ds(pl.multiple_of(k * 128 + m * 16, 16), 16)
            hctx[pl.ds(pl.multiple_of(m * 16, 16), 16), :] = (cn[at, :] * scale1 + shift1).astype(BF16)
            return carry

        lax.fori_loop(0, 8, mod, 0)
        found = jnp.dot(hctx[...], wall[:, 128:512], preferred_element_type=F32)
        uctx[pl.ds(pl.multiple_of(k * 128, 128), 128), :] = found.astype(BF16).astype(F32)
        return carry

    lax.fori_loop(0, CTX // 128, context_chunk, 0)
    context_mixed = conv(uctx[:, :256], jnp.zeros((1, 256), F32), jnp.zeros((1, 256), F32))
    context_values = context_mixed[:, :128]
    context_writes = context_mixed[:, 128:192]
    chunks = CTX // 128
    c_size = [own_steps(uctx[128 * c : 128 * c + 128, 256:384]) for c in range(chunks)]
    c_decay = [-size * rates for size in c_size]
    c_total = [jnp.sum(decay, axis=1, keepdims=True) for decay in c_decay]
    later = jnp.where(ri > ci, 1.0, 0.0)
    earlier = jnp.where(ri < ci, 1.0, 0.0)
    context_state = [jnp.zeros((64, 128), F32), jnp.zeros((64, 128), F32)]
    for c in range(chunks):
        after_it = sum(c_total[c + 1 :], jnp.zeros((8, 1), F32))
        before_it = sum(c_total[:c], jnp.zeros((8, 1), F32))
        rest = jnp.where(
            k8 < 2, dot_f32(c_decay[c], later) + after_it, dot_f32(c_decay[c], earlier) + before_it
        )
        turned = jnp.concatenate([jnp.exp(rest) * c_size[c], jnp.zeros((120, 128), F32)], axis=0).T
        at = slice(128 * c, 128 * c + 128)
        for d in range(2):
            context_state[d] = context_state[d] + state_of(
                context_writes[at], context_values[at] * head_columns(turned, 0, d)
            )
    for d in range(2):
        cst[8 * d : 8 * d + 8] = context_state[d].reshape(8, 8, 128)

    l2_wait()
    s2_wait()
    place = a + direction * (NA - 1 - 2 * a)

    def enter(k, state):
        j = k + direction * (NA - 1 - 2 * k)
        logs = rl2[j]
        factor = jnp.exp(jnp.where(direction == 0, logs[0:1, :], logs[1:2, :]))
        return jnp.where(k < place, factor * state + rs2[j], state)

    entering = lax.fori_loop(0, NA, enter, cst[i])

    def hand_out(k, carry):
        osend[k] = cpre[k] + ppre[k] * entering
        return carry

    lax.fori_loop(0, NI, hand_out, 0)
    s3_start, s3_wait, s3_left = exchange(NI, i, near, lambda j: osend.at[j], rs3, near_ssem.at[3], near_rsem.at[3])
    s3_start()
    rs3[i] = osend[i]
    s3_wait()

    mixer = local
    for d in range(2):
        came = rs3[8 * d : 8 * d + 8].reshape(64, 128)
        mixer = mixer + dot_bf16(reads, came) * head_columns(columns, 16, d)
    gated = mixer * gates
    gated = gated * lax.rsqrt(jnp.mean(gated * gated, axis=-1, keepdims=True) + EPSILON) * ggain[...]
    gated = gated.astype(BF16)
    loads[6].wait()
    for n in range(4):
        at = slice(512 * n, 512 * n + 512)
        oo[:, :, at] = (
            jnp.dot(gated, outw_v[:, at], preferred_element_type=F32).astype(BF16).reshape(NT, ROWS, 512)
        )
    o_start, o_wait, o_left = exchange(NT, t, along_tp, lambda j: oo.at[j], ro, tp_ssem.at[2], tp_rsem.at[2])
    o_start()
    ro[t] = oo[t]
    gate0 = vector(0, 2)
    o_wait()
    summed = ro[0].astype(F32)
    for j in range(1, NT):
        summed = summed + ro[j].astype(F32)
    normed_out = (
        summed * lax.rsqrt(jnp.mean(summed * summed, axis=-1, keepdims=True) + EPSILON) * pgain[...]
    )
    out[...] = (latent[...].astype(F32) + gate0 * normed_out).astype(BF16)

    for left in (m1_left, m2_left, m3_left, m4_left, x_left, l1_left, l2_left, s1_left, s2_left, s3_left, o_left):
        left()
    up.wait_send()
    down.wait_send()


def body(
    latent,
    context,
    condition,
    context_condition,
    modulation_weight,
    norm_gain,
    gate_weight,
    value_weight,
    write_weight,
    read_weight,
    step_weight,
    value_taps,
    map_taps,
    decay_rate,
    decay_jump,
    skip_gain,
    group_gain,
    output_weight,
    post_gain,
):
    vmem = pl.BlockSpec(memory_space=pltpu.VMEM)
    smem = pl.BlockSpec(memory_space=pltpu.SMEM)
    hbm = pl.BlockSpec(memory_space=pl.ANY)
    dma = pltpu.SemaphoreType.DMA
    return pl.pallas_call(
        kernel,
        out_shape=jax.ShapeDtypeStruct((ROWS, D), BF16),
        in_specs=[vmem, vmem, vmem, vmem, vmem, vmem, vmem, smem, vmem, smem, vmem, vmem] + [hbm] * 7,
        out_specs=vmem,
        scratch_shapes=[
            pltpu.VMEM((CTX, D), BF16),
            pltpu.VMEM((D, 64), BF16),
            pltpu.VMEM((D, 64), BF16),
            pltpu.VMEM((D, 32), BF16),
            pltpu.VMEM((128, D), BF16),
            pltpu.VMEM((D, 512), BF16),
            pltpu.VMEM((NY, 4, 128), F32),
            pltpu.VMEM((NI, 4, 128), F32),
            pltpu.VMEM((4, 128), F32),
            pltpu.VMEM((NA, 4, 128), F32),
            pltpu.VMEM((NY, 4, 128), F32),
            pltpu.VMEM((NT, NY, 4, 128), F32),
            pltpu.VMEM((NT + 2, ROWS, D), BF16),
            pltpu.VMEM((NT + 2, ROWS, D), F32),
            pltpu.VMEM((CTX, D), F32),
            pltpu.VMEM(((NT + 2) * ROWS, D), BF16),
            pltpu.VMEM((128, D), BF16),
            pltpu.VMEM((CTX, 384), F32),
            pltpu.VMEM((2, 128), F32),
            pltpu.VMEM((NI, 2, 128), F32),
            pltpu.VMEM((2, 128), F32),
            pltpu.VMEM((NA, 2, 128), F32),
            pltpu.VMEM((NI, 8, 128), F32),
            pltpu.VMEM((NI, 8, 128), F32),
            pltpu.VMEM((8, 128), F32),
            pltpu.VMEM((NA, 8, 128), F32),
            pltpu.VMEM((NI, 8, 128), F32),
            pltpu.VMEM((NI, 1, 128), F32),
            pltpu.VMEM((NI, 8, 128), F32),
            pltpu.VMEM((NI, 8, 128), F32),
            pltpu.VMEM((NI, 8, 128), F32),
            pltpu.VMEM((NT, ROWS, D), BF16),
            pltpu.VMEM((NT, ROWS, D), BF16),
            dma((7,)),
            dma((4, NI)),
            dma((4, NI)),
            dma((3, NA)),
            dma((3, NA)),
            dma((3, NT)),
            dma((3, NT)),
            dma((NY,)),
            dma((NY,)),
            dma((2,)),
            dma((2,)),
        ],
        compiler_params=pltpu.CompilerParams(
            collective_id=0, has_side_effects=True, vmem_limit_bytes=60 * 1024 * 1024
        ),
    )(
        latent,
        condition.reshape(16, 128),
        context_condition.reshape(16, 128),
        modulation_weight.reshape(ROWS, 768),
        norm_gain.reshape(1, D),
        value_taps,
        map_taps,
        decay_rate,
        decay_jump,
        skip_gain,
        group_gain.reshape(1, 128),
        post_gain.reshape(1, D),
        context,
        gate_weight,
        value_weight,
        write_weight,
        read_weight,
        step_weight.reshape(D, 32),
        output_weight,
    )


def solution(mesh):
    torus = Mesh(mesh.devices.reshape(NA, NB, NY, NT), SP_TP)
    return jax.shard_map(
        body,
        mesh=torus,
        in_specs=(
            P(SP_TP, None),
            P(),
            P(),
            P(),
            P(SP, None, "tp"),
            P(),
            P(None, "tp"),
            P(None, "tp"),
            P(None, "tp"),
            P(None, "tp"),
            P(),
            P(None, "tp"),
            P(None, None, "tp"),
            P(),
            P(None, "tp", SP),
            P(),
            P("tp"),
            P("tp", None),
            P(),
        ),
        out_specs=P(SP_TP, None),
        check_vma=False,
    )
```

```python
import jax
import jax.numpy as jnp
from jax import lax
from jax.experimental import pallas as pl
from jax.experimental.pallas import tpu as pltpu
from jax.sharding import Mesh
from jax.sharding import PartitionSpec as P

SP = ("za", "zb", "y")
SP_TP = ("za", "zb", "y", "tp")
MESH = pl.DeviceIdType.MESH
EPSILON = 1e-06
HIGHEST = lax.Precision.HIGHEST
F32 = jnp.float32
BF16 = jnp.bfloat16
NA, NB, NY, NT = 8, 4, 4, 8
NI = NB * NY
NS = NA * NI
D = 2048
ROWS = 16
RANGE = 128
CTX = 512


def silu(x):
    return x * (1.0 / (1.0 + jnp.exp(-x)))


def softplus(x):
    return jnp.maximum(x, 0.0) + jnp.log1p(jnp.exp(-jnp.abs(x)))


def dot_f32(x, y):
    return jnp.dot(x, y, precision=HIGHEST, preferred_element_type=F32)


def dot_bf16(x, y):
    return jnp.dot(x.astype(BF16), y.astype(BF16), preferred_element_type=F32)


def iota(shape, dim):
    return lax.broadcasted_iota(jnp.int32, shape, dim)


def kernel(
    latent_h,
    cond_h,
    ccond_h,
    modw_h,
    ngain_h,
    vtaps_h,
    mtaps_h,
    rate_h,
    jump_h,
    skip_h,
    ggain_h,
    pgain_h,
    context_h,
    gate_h,
    value_h,
    write_h,
    read_h,
    step_h,
    outw_h,
    out,
    latent,
    cond,
    ccond,
    modw,
    ngain,
    vtaps,
    mtaps,
    rate,
    jump,
    skip,
    ggain,
    pgain,
    context_v,
    rest_v,
    outw_v,
    wall,
    part,
    r1,
    s1,
    r2,
    s2,
    r4,
    xg,
    hsend,
    hrecv,
    xn,
    cn,
    hid,
    hctx,
    uctx,
    lsend,
    rl1,
    l2send,
    rl2,
    sp,
    rs1,
    bt,
    rs2,
    cpre,
    ppre,
    cst,
    osend,
    rs3,
    oo,
    ro,
    small_sem,
    load_sem,
    near_ssem,
    near_rsem,
    far_ssem,
    far_rsem,
    tp_ssem,
    tp_rsem,
    plane_ssem,
    plane_rsem,
    halo_ssem,
    halo_rsem,
):
    a = lax.axis_index("za")
    b = lax.axis_index("zb")
    y = lax.axis_index("y")
    t = lax.axis_index("tp")
    i = b * NY + y
    s = a * NI + i
    g = y * NT + t
    direction = lax.div(i, 8)

    def near(j):
        return {"zb": lax.div(j, NY), "y": lax.rem(j, NY)}

    def far(j):
        return {"za": j}

    def plane(j):
        return {"y": lax.div(j, NT), "tp": lax.rem(j, NT)}

    def along_tp(j):
        return {"tp": j}

    def at_range(n):
        return {"za": lax.div(n, NI), "zb": lax.div(lax.rem(n, NI), NY), "y": lax.rem(n, NY)}

    following = at_range(lax.rem(s + 1, NS))
    preceding = at_range(lax.rem(s + NS - 1, NS))

    def copy(src, dst, ssem, rsem, device):
        return pltpu.make_async_remote_copy(
            src_ref=src, dst_ref=dst, send_sem=ssem, recv_sem=rsem, device_id=device, device_id_type=MESH
        )

    def exchange(n, me, peer, src_of, dst, ssem, rsem):
        def begin(k, carry):
            j = lax.rem(me + k, n)
            copy(src_of(j), dst.at[me], ssem.at[k], rsem.at[me], peer(j)).start()
            return carry

        def arrive(k, carry):
            j = lax.rem(me + n - k, n)
            copy(src_of(j), dst.at[j], ssem.at[k], rsem.at[j], peer(j)).wait_recv()
            return carry

        def leave(k, carry):
            j = lax.rem(me + k, n)
            copy(src_of(j), dst.at[me], ssem.at[k], rsem.at[me], peer(j)).wait_send()
            return carry

        return (
            lambda: lax.fori_loop(1, n, begin, 0),
            lambda: lax.fori_loop(1, n, arrive, 0),
            lambda: lax.fori_loop(1, n, leave, 0),
        )

    barrier = pltpu.get_barrier_semaphore()

    def tell(device):
        pl.semaphore_signal(barrier, inc=1, device_id=device, device_id_type=MESH)

    def tell_all(n, me, peer):
        def one(k, carry):
            tell(peer(lax.rem(me + k, n)))
            return carry

        lax.fori_loop(1, n, one, 0)

    tell_all(NA, a, far)
    tell_all(NI, i, near)
    tell_all(NY * NT, g, plane)
    tell(following)
    tell(preceding)

    small = [
        pltpu.make_async_copy(src, dst, small_sem.at[n])
        for n, (src, dst) in enumerate(
            (
                (cond_h, cond),
                (ccond_h, ccond),
                (modw_h, modw),
                (latent_h, latent),
                (ngain_h, ngain),
                (vtaps_h, vtaps),
                (mtaps_h, mtaps),
                (rate_h, rate),
                (jump_h, jump),
                (skip_h, skip),
                (ggain_h, ggain),
                (pgain_h, pgain),
            )
        )
    ]
    for load in small:
        load.start()
    loads = [
        pltpu.make_async_copy(gate_h, wall.at[:, pl.ds(0, 128)], load_sem.at[0]),
        pltpu.make_async_copy(value_h, wall.at[:, pl.ds(128, 128)], load_sem.at[1]),
        pltpu.make_async_copy(write_h, rest_v.at[pl.ds(0, 64)], load_sem.at[2]),
        pltpu.make_async_copy(read_h, rest_v.at[pl.ds(64, 64)], load_sem.at[3]),
        pltpu.make_async_copy(step_h, rest_v.at[pl.ds(128, 32)], load_sem.at[4]),
        pltpu.make_async_copy(context_h, context_v, load_sem.at[5]),
        pltpu.make_async_copy(outw_h, outw_v, load_sem.at[6]),
    ]
    for load in loads:
        load.start()
    for load in small:
        load.wait()

    lane = iota((1, 128), 1)
    mine = lax.div(lane, ROWS) == lax.rem(s, 8)
    rows8 = iota((8, 128), 0)
    first = jnp.where(mine, silu(cond[pl.ds(lax.div(s, 8), 1), :]), 0.0)
    second = jnp.where(mine, silu(ccond[pl.ds(lax.div(s, 8), 1), :]), 0.0)
    both = jnp.where(rows8 == 0, first, jnp.where(rows8 == 1, second, 0.0))
    weight = jnp.concatenate([modw[k].astype(F32) for k in range(3)], axis=1)
    pieces = dot_f32(both, jnp.concatenate([weight] * 8, axis=0))
    for m in range(12):
        r, k, half = m // 6, (m % 6) // 2, m % 2
        low = k * 256 + half * 128
        part[m // 3, m % 3 : m % 3 + 1, :] = pieces[r : r + 1, low : low + 128]

    m1_start, m1_wait, m1_left = exchange(
        NI, i, near, lambda j: part.at[lax.rem(j, NY)], r1, near_ssem.at[0], near_rsem.at[0]
    )
    m2_start, m2_wait, m2_left = exchange(NA, a, far, lambda j: s1, r2, far_ssem.at[0], far_rsem.at[0])
    m3_start, m3_wait, m3_left = exchange(NY * NT, g, plane, lambda j: s2, r4, plane_ssem, plane_rsem)
    x_start, x_wait, x_left = exchange(NT, t, along_tp, lambda j: latent, xg, tp_ssem.at[0], tp_rsem.at[0])

    pl.semaphore_wait(barrier, (NA - 1) + (NI - 1) + (NY * NT - 1) + 2)

    m1_start()
    r1[i] = part[y]
    x_start()
    xg[t] = latent[...]

    for load in loads[:5]:
        load.wait()

    rest_v[160:256, :] = jnp.zeros((96, D), BF16)

    def join(k, carry):
        at = pl.ds(pl.multiple_of(k * 256, 256), 256)
        wall[at, 256:512] = rest_v[:, at].T
        return carry

    lax.fori_loop(0, D // 256, join, 0)

    m1_wait()
    s1[...] = jnp.sum(r1[...], axis=0)
    m2_start()
    r2[a] = s1[...]

    x_wait()
    hsend[0] = xg[NT - 1].astype(F32)[15:16, :]
    hsend[1] = xg[0].astype(F32)[0:1, :]
    up = copy(hsend.at[0], hrecv.at[0], halo_ssem.at[0], halo_rsem.at[0], following)
    down = copy(hsend.at[1], hrecv.at[1], halo_ssem.at[1], halo_rsem.at[1], preceding)
    up.start()
    down.start()
    gain = ngain[...]

    def normed(x):
        return x * lax.rsqrt(jnp.mean(x * x, axis=-1, keepdims=True) + EPSILON) * gain

    def norm_latent(k, carry):
        xn[k] = normed(xg[k].astype(F32))
        return carry

    lax.fori_loop(0, NT, norm_latent, 0)
    up.wait_recv()
    down.wait_recv()
    xn[NT] = jnp.concatenate([normed(hrecv[0]), normed(hrecv[1]), jnp.zeros((14, D), F32)], axis=0)
    loads[5].wait()

    def norm_context(k, carry):
        at = pl.ds(pl.multiple_of(k * 16, 16), 16)
        cn[at, :] = normed(context_v[at, :].astype(F32))
        return carry

    lax.fori_loop(0, CTX // 16, norm_context, 0)

    m2_wait()
    s2[...] = jnp.sum(r2[...], axis=0)
    m3_start()
    r4[g] = s2[...]
    m3_wait()

    def vector(r, k):
        found = []
        for j in range(NT):
            for half in range(2):
                m = (r * 3 + k) * 2 + half
                found.append(r4[m // 3 * NT + j, m % 3 : m % 3 + 1, :])
        return jnp.concatenate(found, axis=1)

    shift0, scale0 = vector(0, 0), 1.0 + vector(0, 1)

    def modulate(k, carry):
        hid[pl.ds(pl.multiple_of(k * 16, 16), 16), :] = (xn[k] * scale0 + shift0).astype(BF16)
        return carry

    lax.fori_loop(0, NT + 1, modulate, 0)
    linear = jnp.dot(hid[...], wall[...], preferred_element_type=F32).astype(BF16).astype(F32)
    gate_linear = linear[:RANGE, :128]
    u = linear[:RANGE, 128:384]
    step_linear = linear[:RANGE, 384:512]
    before = jnp.where(s > 0, linear[RANGE : RANGE + 1, 128:384], 0.0)
    after = jnp.where(s < NS - 1, linear[RANGE + 1 : RANGE + 2, 128:384], 0.0)
    vt = vtaps[...].astype(F32)

    def taps(k):
        m = mtaps[k].astype(F32)
        return jnp.concatenate([vt[k : k + 1, :], m[0:1, :], m[1:2, :]], axis=1)

    tap = [taps(k) for k in range(3)]

    def conv(u, before, after):
        n = u.shape[0]
        row = iota(u.shape, 0)
        lower = jnp.where(row == 0, before, pltpu.roll(u, 1, 0))
        upper = jnp.where(row == n - 1, after, pltpu.roll(u, n - 1, 0))
        return silu(tap[0] * lower + tap[1] * u + tap[2] * upper)

    k8 = iota((8, 128), 0)
    lane8 = iota((8, 128), 1)
    chosen = jnp.where((k8 < 4) & (lane8 == lax.div(k8, 2) * 16 + 2 * t + lax.rem(k8, 2)), 1.0, 0.0)

    def own_steps(step_linear):
        return softplus(
            lax.dot_general(
                chosen.astype(BF16),
                step_linear.astype(BF16),
                (((1,), (1,)), ((), ())),
                preferred_element_type=F32,
            )
        )

    rates = jnp.zeros((8, 128), F32)
    lane16 = iota((1, 16), 1)

    def own(row, h):
        return jnp.sum(jnp.where(lane16 == 2 * t + h, row, 0.0), axis=1, keepdims=True)

    for k in range(4):
        rates = jnp.where(k8 == k, own(rate[k // 2 : k // 2 + 1, :], k % 2), rates)
    jumps = jnp.concatenate([jump[0], jump[1], jnp.zeros((4, 128), F32)], axis=0)
    size_row = own_steps(step_linear)
    decay_row = jumps - size_row * rates
    ri = iota((128, 128), 0)
    ci = iota((128, 128), 1)
    upto = jnp.where(ri <= ci, 1.0, 0.0)
    onwards = jnp.where(ri >= ci, 1.0, 0.0)
    within_row = jnp.where(k8 < 2, dot_f32(decay_row, upto), dot_f32(decay_row, onwards))
    total = jnp.sum(decay_row, axis=1, keepdims=True)
    low_lanes = lane < 64

    def total_lanes(d):
        return jnp.where(low_lanes, total[2 * d : 2 * d + 1, :], total[2 * d + 1 : 2 * d + 2, :])

    lsend[0:1, :] = total_lanes(0)
    lsend[1:2, :] = total_lanes(1)
    l1_start, l1_wait, l1_left = exchange(NI, i, near, lambda j: lsend, rl1, near_ssem.at[1], near_rsem.at[1])
    l1_start()
    rl1[i] = lsend[...]

    columns = jnp.concatenate(
        [within_row, jnp.exp(total - within_row) * size_row, jnp.exp(within_row), jnp.zeros((104, 128), F32)],
        axis=0,
    ).T

    def head_columns(columns, base, d):
        at = base + 2 * d
        return jnp.where(low_lanes, columns[:, at : at + 1], columns[:, at + 1 : at + 2])

    mixed = conv(u, before, after)
    values = mixed[:, :128]
    writes = mixed[:, 128:192].astype(BF16)
    reads = mixed[:, 192:256].astype(BF16)

    def state_of(writes, weighted):
        return lax.dot_general(
            writes.astype(BF16),
            weighted.astype(BF16),
            (((0,), (0,)), ((), ())),
            preferred_element_type=F32,
        )

    for d in range(2):
        sp[8 * d : 8 * d + 8] = state_of(writes, values * head_columns(columns, 8, d)).astype(BF16).reshape(8, 8, 128)
    s1_start, s1_wait, s1_left = exchange(NI, i, near, lambda j: sp.at[j], rs1, near_ssem.at[2], near_rsem.at[2])
    s1_start()
    rs1[i] = sp[i]

    scores = lax.dot_general(reads, writes, (((1,), (1,)), ((), ())), preferred_element_type=F32)
    inner = []
    for h in range(2):
        fading = jnp.zeros((128, 128), F32)
        for d in range(2):
            k = 2 * d + h
            gap = columns[:, k : k + 1] - within_row[k : k + 1, :]
            mask = (ri >= ci) if d == 0 else (ri <= ci)
            fading = fading + jnp.exp(jnp.where(mask, gap, -1e30)) * size_row[k : k + 1, :]
        inner.append(dot_bf16(scores * fading, values[:, 64 * h : 64 * h + 64]))
    skips = jnp.where(low_lanes, own(skip[...], 0), own(skip[...], 1))
    local = skips * values + jnp.concatenate(inner, axis=1)
    gates = silu(gate_linear)

    l1_wait()
    l2send[...] = jnp.sum(rl1[...], axis=0)
    l2_start, l2_wait, l2_left = exchange(NA, a, far, lambda j: l2send, rl2, far_ssem.at[1], far_rsem.at[1])
    l2_start()
    rl2[a] = l2send[...]

    s1_wait()

    def fold(k, carry):
        state, product = carry
        j = k + direction * (NI - 1 - 2 * k)
        cpre[j] = state
        ppre[j] = product
        logs = rl1[j]
        factor = jnp.exp(jnp.where(direction == 0, logs[0:1, :], logs[1:2, :]))
        return factor * state + rs1[j].astype(F32), factor * product

    block_state, _ = lax.fori_loop(
        0, NI, fold, (jnp.zeros((8, 128), F32), jnp.ones((1, 128), F32))
    )
    bt[...] = block_state.astype(BF16)
    s2_start, s2_wait, s2_left = exchange(NA, a, far, lambda j: bt, rs2, far_ssem.at[2], far_rsem.at[2])
    s2_start()
    rs2[a] = bt[...]

    shift1, scale1 = vector(1, 0), 1.0 + vector(1, 1)

    def context_chunk(k, carry):
        def mod(m, carry):
            at = pl.ds(pl.multiple_of(k * 128 + m * 16, 16), 16)
            hctx[pl.ds(pl.multiple_of(m * 16, 16), 16), :] = (cn[at, :] * scale1 + shift1).astype(BF16)
            return carry

        lax.fori_loop(0, 8, mod, 0)
        found = jnp.dot(hctx[...], wall[:, 128:512], preferred_element_type=F32)
        uctx[pl.ds(pl.multiple_of(k * 128, 128), 128), :] = found.astype(BF16).astype(F32)
        return carry

    lax.fori_loop(0, CTX // 128, context_chunk, 0)
    context_mixed = conv(uctx[:, :256], jnp.zeros((1, 256), F32), jnp.zeros((1, 256), F32))
    context_values = context_mixed[:, :128]
    context_writes = context_mixed[:, 128:192]
    chunks = CTX // 128
    c_size = [own_steps(uctx[128 * c : 128 * c + 128, 256:384]) for c in range(chunks)]
    c_decay = [-size * rates for size in c_size]
    c_total = [jnp.sum(decay, axis=1, keepdims=True) for decay in c_decay]
    later = jnp.where(ri > ci, 1.0, 0.0)
    earlier = jnp.where(ri < ci, 1.0, 0.0)
    context_state = [jnp.zeros((64, 128), F32), jnp.zeros((64, 128), F32)]
    for c in range(chunks):
        after_it = sum(c_total[c + 1 :], jnp.zeros((8, 1), F32))
        before_it = sum(c_total[:c], jnp.zeros((8, 1), F32))
        rest = jnp.where(
            k8 < 2, dot_f32(c_decay[c], later) + after_it, dot_f32(c_decay[c], earlier) + before_it
        )
        turned = jnp.concatenate([jnp.exp(rest) * c_size[c], jnp.zeros((120, 128), F32)], axis=0).T
        at = slice(128 * c, 128 * c + 128)
        for d in range(2):
            context_state[d] = context_state[d] + state_of(
                context_writes[at], context_values[at] * head_columns(turned, 0, d)
            )
    for d in range(2):
        cst[8 * d : 8 * d + 8] = context_state[d].reshape(8, 8, 128)

    for left in (m1_left, m2_left, m3_left, x_left, l1_left, s1_left, l2_left, s2_left):
        left()
    up.wait_send()
    down.wait_send()
    l2_wait()
    s2_wait()
    place = a + direction * (NA - 1 - 2 * a)

    def enter(k, state):
        j = k + direction * (NA - 1 - 2 * k)
        logs = rl2[j]
        factor = jnp.exp(jnp.where(direction == 0, logs[0:1, :], logs[1:2, :]))
        return jnp.where(k < place, factor * state + rs2[j].astype(F32), state)

    entering = lax.fori_loop(0, NA, enter, cst[i])

    def hand_out(k, carry):
        osend[k] = (cpre[k] + ppre[k] * entering).astype(BF16)
        return carry

    lax.fori_loop(0, NI, hand_out, 0)
    s3_start, s3_wait, s3_left = exchange(NI, i, near, lambda j: osend.at[j], rs3, near_ssem.at[3], near_rsem.at[3])
    s3_start()
    rs3[i] = osend[i]
    s3_wait()

    mixer = local
    for d in range(2):
        came = rs3[8 * d : 8 * d + 8].reshape(64, 128)
        mixer = mixer + dot_bf16(reads, came) * head_columns(columns, 16, d)
    gated = mixer * gates
    gated = gated * lax.rsqrt(jnp.mean(gated * gated, axis=-1, keepdims=True) + EPSILON) * ggain[...]
    gated = gated.astype(BF16)
    loads[6].wait()
    for n in range(4):
        at = slice(512 * n, 512 * n + 512)
        oo[:, :, at] = (
            jnp.dot(gated, outw_v[:, at], preferred_element_type=F32).astype(BF16).reshape(NT, ROWS, 512)
        )
    o_start, o_wait, o_left = exchange(NT, t, along_tp, lambda j: oo.at[j], ro, tp_ssem.at[2], tp_rsem.at[2])
    o_start()
    ro[t] = oo[t]
    gate0 = vector(0, 2)
    o_wait()
    summed = ro[0].astype(F32)
    for j in range(1, NT):
        summed = summed + ro[j].astype(F32)
    normed_out = (
        summed * lax.rsqrt(jnp.mean(summed * summed, axis=-1, keepdims=True) + EPSILON) * pgain[...]
    )
    out[...] = (latent[...].astype(F32) + gate0 * normed_out).astype(BF16)

    s3_left()
    o_left()


def body(
    latent,
    context,
    condition,
    context_condition,
    modulation_weight,
    norm_gain,
    gate_weight,
    value_weight,
    write_weight,
    read_weight,
    step_weight,
    value_taps,
    map_taps,
    decay_rate,
    decay_jump,
    skip_gain,
    group_gain,
    output_weight,
    post_gain,
):
    vmem = pl.BlockSpec(memory_space=pltpu.VMEM)
    hbm = pl.BlockSpec(memory_space=pl.ANY)
    dma = pltpu.SemaphoreType.DMA
    return pl.pallas_call(
        kernel,
        out_shape=jax.ShapeDtypeStruct((ROWS, D), BF16),
        in_specs=[hbm] * 19,
        out_specs=vmem,
        scratch_shapes=[
            pltpu.VMEM((ROWS, D), BF16),
            pltpu.VMEM((16, 128), F32),
            pltpu.VMEM((16, 128), F32),
            pltpu.VMEM((3, ROWS, 256), BF16),
            pltpu.VMEM((1, D), F32),
            pltpu.VMEM((3, 128), BF16),
            pltpu.VMEM((3, 2, 64), BF16),
            pltpu.VMEM((2, 16), F32),
            pltpu.VMEM((2, 2, 128), F32),
            pltpu.VMEM((1, 16), F32),
            pltpu.VMEM((1, 128), F32),
            pltpu.VMEM((1, D), F32),
            pltpu.VMEM((CTX, D), BF16),
            pltpu.VMEM((256, D), BF16),
            pltpu.VMEM((128, D), BF16),
            pltpu.VMEM((D, 512), BF16),
            pltpu.VMEM((NY, 4, 128), F32),
            pltpu.VMEM((NI, 4, 128), F32),
            pltpu.VMEM((4, 128), F32),
            pltpu.VMEM((NA, 4, 128), F32),
            pltpu.VMEM((4, 128), F32),
            pltpu.VMEM((NY * NT, 4, 128), F32),
            pltpu.VMEM((NT, ROWS, D), BF16),
            pltpu.VMEM((2, 1, D), F32),
            pltpu.VMEM((2, 1, D), F32),
            pltpu.VMEM((NT + 1, ROWS, D), F32),
            pltpu.VMEM((CTX, D), F32),
            pltpu.VMEM(((NT + 1) * ROWS, D), BF16),
            pltpu.VMEM((128, D), BF16),
            pltpu.VMEM((CTX, 384), F32),
            pltpu.VMEM((2, 128), F32),
            pltpu.VMEM((NI, 2, 128), F32),
            pltpu.VMEM((2, 128), F32),
            pltpu.VMEM((NA, 2, 128), F32),
            pltpu.VMEM((NI, 8, 128), BF16),
            pltpu.VMEM((NI, 8, 128), BF16),
            pltpu.VMEM((8, 128), BF16),
            pltpu.VMEM((NA, 8, 128), BF16),
            pltpu.VMEM((NI, 8, 128), F32),
            pltpu.VMEM((NI, 1, 128), F32),
            pltpu.VMEM((NI, 8, 128), F32),
            pltpu.VMEM((NI, 8, 128), BF16),
            pltpu.VMEM((NI, 8, 128), BF16),
            pltpu.VMEM((NT, ROWS, D), BF16),
            pltpu.VMEM((NT, ROWS, D), BF16),
            dma((12,)),
            dma((7,)),
            dma((4, NI)),
            dma((4, NI)),
            dma((3, NA)),
            dma((3, NA)),
            dma((3, NT)),
            dma((3, NT)),
            dma((NY * NT,)),
            dma((NY * NT,)),
            dma((2,)),
            dma((2,)),
        ],
        compiler_params=pltpu.CompilerParams(
            collective_id=0, has_side_effects=True, vmem_limit_bytes=60 * 1024 * 1024
        ),
    )(
        latent,
        condition.reshape(16, 128),
        context_condition.reshape(16, 128),
        modulation_weight.transpose(1, 0, 2),
        norm_gain.reshape(1, D),
        value_taps,
        map_taps,
        decay_rate,
        decay_jump,
        skip_gain.reshape(1, 16),
        group_gain.reshape(1, 128),
        post_gain.reshape(1, D),
        context,
        gate_weight,
        value_weight,
        write_weight.T,
        read_weight.T,
        step_weight.transpose(1, 2, 0).reshape(32, D),
        output_weight,
    )


def solution(mesh):
    torus = Mesh(mesh.devices.reshape(NA, NB, NY, NT), SP_TP)
    return jax.shard_map(
        body,
        mesh=torus,
        in_specs=(
            P(SP_TP, None),
            P(),
            P(),
            P(),
            P(SP, None, "tp"),
            P(),
            P(None, "tp"),
            P(None, "tp"),
            P(None, "tp"),
            P(None, "tp"),
            P(),
            P(None, "tp"),
            P(None, None, "tp"),
            P(),
            P(None, "tp", SP),
            P(),
            P("tp"),
            P("tp", None),
            P(),
        ),
        out_specs=P(SP_TP, None),
        check_vma=False,
    )
```

```python
import jax
import jax.numpy as jnp
from jax import lax
from jax.experimental import pallas as pl
from jax.experimental.pallas import tpu as pltpu
from jax.sharding import Mesh
from jax.sharding import PartitionSpec as P

SP = ("za", "zb", "y")
SP_TP = ("za", "zb", "y", "tp")
MESH = pl.DeviceIdType.MESH
EPSILON = 1e-06
HIGHEST = lax.Precision.HIGHEST
F32 = jnp.float32
BF16 = jnp.bfloat16
NA, NB, NY, NT = 8, 4, 4, 8
NI = NB * NY
NS = NA * NI
D = 2048
ROWS = 16
RANGE = 128
CTX = 512


def silu(x):
    return x * (1.0 / (1.0 + jnp.exp(-x)))


def softplus(x):
    return jnp.maximum(x, 0.0) + jnp.log1p(jnp.exp(-jnp.abs(x)))


def dot_f32(x, y):
    return jnp.dot(x, y, precision=HIGHEST, preferred_element_type=F32)


def dot_bf16(x, y):
    return jnp.dot(x.astype(BF16), y.astype(BF16), preferred_element_type=F32)


def iota(shape, dim):
    return lax.broadcasted_iota(jnp.int32, shape, dim)


def kernel(
    latent_h,
    cond_h,
    ccond_h,
    modw_h,
    ngain_h,
    vtaps_h,
    mtaps_h,
    rate_h,
    jump_h,
    skip_h,
    ggain_h,
    pgain_h,
    context_h,
    gate_h,
    value_h,
    write_h,
    read_h,
    step_h,
    outw_h,
    out,
    latent,
    cond,
    ccond,
    modw,
    ngain,
    vtaps,
    mtaps,
    rate,
    jump,
    skip,
    ggain,
    pgain,
    context_v,
    rest_v,
    outw_v,
    wall,
    part,
    r1,
    r2,
    s2,
    r4,
    xg,
    hsend,
    hrecv,
    xn,
    cn,
    hid,
    hctx,
    uctx,
    lsend,
    rl1,
    l2send,
    rl2,
    sp,
    rs1,
    bt,
    rs2,
    cpre,
    ppre,
    cst,
    osend,
    rs3,
    oo,
    ro,
    small_sem,
    load_sem,
    near_ssem,
    near_rsem,
    far_ssem,
    far_rsem,
    tp_ssem,
    tp_rsem,
    plane_ssem,
    plane_rsem,
    ring_ssem,
    ring_rsem,
    halo_ssem,
    halo_rsem,
):
    a = lax.axis_index("za")
    b = lax.axis_index("zb")
    y = lax.axis_index("y")
    t = lax.axis_index("tp")
    i = b * NY + y
    s = a * NI + i
    g = y * NT + t
    direction = lax.div(i, 8)

    def near(j):
        return {"zb": lax.div(j, NY), "y": lax.rem(j, NY)}

    def far(j):
        return {"za": j}

    def plane(j):
        return {"y": lax.div(j, NT), "tp": lax.rem(j, NT)}

    def along_tp(j):
        return {"tp": j}

    def at_range(n):
        return {"za": lax.div(n, NI), "zb": lax.div(lax.rem(n, NI), NY), "y": lax.rem(n, NY)}

    following = at_range(lax.rem(s + 1, NS))
    preceding = at_range(lax.rem(s + NS - 1, NS))
    next_block = {"za": lax.rem(a + 1, NA)}
    last_block = {"za": lax.rem(a + NA - 1, NA)}

    def copy(src, dst, ssem, rsem, device):
        return pltpu.make_async_remote_copy(
            src_ref=src, dst_ref=dst, send_sem=ssem, recv_sem=rsem, device_id=device, device_id_type=MESH
        )

    def exchange(n, me, peer, src_of, dst, ssem, rsem):
        def begin(k, carry):
            j = lax.rem(me + k, n)
            copy(src_of(j), dst.at[me], ssem, rsem, peer(j)).start()
            return carry

        others = dst.at[pl.ds(0, n - 1)]
        return (
            lambda: lax.fori_loop(1, n, begin, 0),
            lambda: pltpu.make_async_copy(others, others, rsem).wait(),
            lambda: pltpu.make_async_copy(others, others, ssem).wait(),
        )

    small = [
        pltpu.make_async_copy(src, dst, small_sem.at[n])
        for n, (src, dst) in enumerate(
            (
                (cond_h, cond),
                (ccond_h, ccond),
                (modw_h, modw),
                (latent_h, latent),
                (ngain_h, ngain),
                (vtaps_h, vtaps),
                (mtaps_h, mtaps),
                (rate_h, rate),
                (jump_h, jump),
                (skip_h, skip),
                (ggain_h, ggain),
                (pgain_h, pgain),
            )
        )
    ]
    for load in small:
        load.start()
    barrier = pltpu.get_barrier_semaphore()

    def tell(device):
        pl.semaphore_signal(barrier, inc=1, device_id=device, device_id_type=MESH)

    def tell_all(n, me, peer):
        def one(k, carry):
            tell(peer(lax.rem(me + k, n)))
            return carry

        lax.fori_loop(1, n, one, 0)

    tell(next_block)
    tell(last_block)
    tell_all(NI, i, near)
    tell_all(NY * NT, g, plane)
    tell(following)
    tell(preceding)

    loads = [
        pltpu.make_async_copy(gate_h, wall.at[:, pl.ds(0, 128)], load_sem.at[0]),
        pltpu.make_async_copy(value_h, wall.at[:, pl.ds(128, 128)], load_sem.at[1]),
        pltpu.make_async_copy(write_h, rest_v.at[pl.ds(0, 64)], load_sem.at[2]),
        pltpu.make_async_copy(read_h, rest_v.at[pl.ds(64, 64)], load_sem.at[3]),
        pltpu.make_async_copy(step_h, rest_v.at[pl.ds(128, 32)], load_sem.at[4]),
        pltpu.make_async_copy(context_h, context_v, load_sem.at[5]),
        pltpu.make_async_copy(outw_h, outw_v, load_sem.at[6]),
    ]
    for load in loads:
        load.start()
    for load in small:
        load.wait()

    lane = iota((1, 128), 1)
    mine = lax.div(lane, ROWS) == lax.rem(s, 8)
    rows8 = iota((8, 128), 0)
    first = jnp.where(mine, silu(cond[pl.ds(lax.div(s, 8), 1), :]), 0.0)
    second = jnp.where(mine, silu(ccond[pl.ds(lax.div(s, 8), 1), :]), 0.0)
    both = jnp.where(rows8 == 0, first, jnp.where(rows8 == 1, second, 0.0))
    weight = jnp.concatenate([modw[k].astype(F32) for k in range(3)], axis=1)
    pieces = dot_f32(both, jnp.concatenate([weight] * 8, axis=0))
    for m in range(12):
        r, k, half = m // 6, (m % 6) // 2, m % 2
        low = k * 256 + half * 128
        part[m // 3, m % 3 : m % 3 + 1, :] = pieces[r : r + 1, low : low + 128]

    m1_start, m1_wait, m1_left = exchange(
        NI, i, near, lambda j: part.at[lax.rem(j, NY)], r1, near_ssem.at[0], near_rsem.at[0]
    )

    def block(k):
        return r2.at[lax.rem(a + k + NA, NA)]

    def relay(k):
        found = [copy(block(1 - k), block(1 - k), ring_ssem.at[k - 1], ring_rsem.at[k - 1], next_block)]
        if k < NA // 2:
            found.append(copy(block(k - 1), block(k - 1), ring_ssem.at[k + 3], ring_rsem.at[k + 3], last_block))
        return found

    def relay_start(k):
        for c in relay(k):
            c.start()

    def relay_wait(k):
        copy(block(-k), block(-k), ring_ssem.at[k - 1], ring_rsem.at[k - 1], next_block).wait_recv()
        if k < NA // 2:
            copy(block(k), block(k), ring_ssem.at[k + 3], ring_rsem.at[k + 3], last_block).wait_recv()

    def relay_left():
        for k in range(1, NA // 2 + 1):
            for c in relay(k):
                c.wait_send()

    m3_start, m3_wait, m3_left = exchange(NY * NT, g, plane, lambda j: s2, r4, plane_ssem.at[0], plane_rsem.at[0])
    x_start, x_wait, x_left = exchange(NT, t, along_tp, lambda j: latent, xg, tp_ssem.at[0], tp_rsem.at[0])

    pl.semaphore_wait(barrier, 2 + (NI - 1) + (NY * NT - 1) + 2)

    m1_start()
    r1[i] = part[y]
    x_start()
    xg[t] = latent[...]

    m1_wait()
    r2[a] = jnp.sum(r1[...], axis=0)
    relay_start(1)

    for load in loads[:5]:
        load.wait()
    rest_v[160:256, :] = jnp.zeros((96, D), BF16)

    def join(k, carry):
        at = pl.ds(pl.multiple_of(k * 256, 256), 256)
        wall[at, 256:512] = rest_v[:, at].T
        return carry

    lax.fori_loop(0, D // 256, join, 0)
    relay_wait(1)
    relay_start(2)

    x_wait()
    hsend[0] = xg[NT - 1].astype(F32)[15:16, :]
    hsend[1] = xg[0].astype(F32)[0:1, :]
    up = copy(hsend.at[0], hrecv.at[0], halo_ssem.at[0], halo_rsem.at[0], following)
    down = copy(hsend.at[1], hrecv.at[1], halo_ssem.at[1], halo_rsem.at[1], preceding)
    up.start()
    down.start()
    gain = ngain[...]

    def normed(x):
        return x * lax.rsqrt(jnp.mean(x * x, axis=-1, keepdims=True) + EPSILON) * gain

    def norm_latent(k, carry):
        xn[k] = normed(xg[k].astype(F32))
        return carry

    lax.fori_loop(0, NT, norm_latent, 0)
    relay_wait(2)
    relay_start(3)

    up.wait_recv()
    down.wait_recv()
    xn[NT] = jnp.concatenate([normed(hrecv[0]), normed(hrecv[1]), jnp.zeros((14, D), F32)], axis=0)
    loads[5].wait()

    def norm_context(k, carry):
        at = pl.ds(pl.multiple_of(k * 16, 16), 16)
        cn[at, :] = normed(context_v[at, :].astype(F32))
        return carry

    lax.fori_loop(0, CTX // 32, norm_context, 0)
    relay_wait(3)
    relay_start(4)
    lax.fori_loop(CTX // 32, CTX // 16, norm_context, 0)
    relay_wait(4)
    s2[...] = jnp.sum(r2[...], axis=0)
    m3_start()
    r4[g] = s2[...]
    m3_wait()

    def vector(r, k):
        found = []
        for j in range(NT):
            for half in range(2):
                m = (r * 3 + k) * 2 + half
                found.append(r4[m // 3 * NT + j, m % 3 : m % 3 + 1, :])
        return jnp.concatenate(found, axis=1)

    shift0, scale0 = vector(0, 0), 1.0 + vector(0, 1)

    def modulate(k, carry):
        hid[pl.ds(pl.multiple_of(k * 16, 16), 16), :] = (xn[k] * scale0 + shift0).astype(BF16)
        return carry

    lax.fori_loop(0, NT + 1, modulate, 0)
    linear = jnp.dot(hid[...], wall[...], preferred_element_type=F32).astype(BF16).astype(F32)
    gate_linear = linear[:RANGE, :128]
    u = linear[:RANGE, 128:384]
    step_linear = linear[:RANGE, 384:512]
    before = jnp.where(s > 0, linear[RANGE : RANGE + 1, 128:384], 0.0)
    after = jnp.where(s < NS - 1, linear[RANGE + 1 : RANGE + 2, 128:384], 0.0)
    vt = vtaps[...].astype(F32)

    def taps(k):
        m = mtaps[k].astype(F32)
        return jnp.concatenate([vt[k : k + 1, :], m[0:1, :], m[1:2, :]], axis=1)

    tap = [taps(k) for k in range(3)]

    def conv(u, before, after):
        n = u.shape[0]
        row = iota(u.shape, 0)
        lower = jnp.where(row == 0, before, pltpu.roll(u, 1, 0))
        upper = jnp.where(row == n - 1, after, pltpu.roll(u, n - 1, 0))
        return silu(tap[0] * lower + tap[1] * u + tap[2] * upper)

    k8 = iota((8, 128), 0)
    lane8 = iota((8, 128), 1)
    chosen = jnp.where((k8 < 4) & (lane8 == lax.div(k8, 2) * 16 + 2 * t + lax.rem(k8, 2)), 1.0, 0.0)

    def own_steps(step_linear):
        return softplus(
            lax.dot_general(
                chosen.astype(BF16),
                step_linear.astype(BF16),
                (((1,), (1,)), ((), ())),
                preferred_element_type=F32,
            )
        )

    rates = jnp.zeros((8, 128), F32)
    lane16 = iota((1, 16), 1)

    def own(row, h):
        return jnp.sum(jnp.where(lane16 == 2 * t + h, row, 0.0), axis=1, keepdims=True)

    for k in range(4):
        rates = jnp.where(k8 == k, own(rate[k // 2 : k // 2 + 1, :], k % 2), rates)
    jumps = jnp.concatenate([jump[0], jump[1], jnp.zeros((4, 128), F32)], axis=0)
    size_row = own_steps(step_linear)
    decay_row = jumps - size_row * rates
    ri = iota((128, 128), 0)
    ci = iota((128, 128), 1)
    upto = jnp.where(ri <= ci, 1.0, 0.0)
    onwards = jnp.where(ri >= ci, 1.0, 0.0)
    within_row = jnp.where(k8 < 2, dot_f32(decay_row, upto), dot_f32(decay_row, onwards))
    total = jnp.sum(decay_row, axis=1, keepdims=True)
    low_lanes = lane < 64

    def total_lanes(d):
        return jnp.where(low_lanes, total[2 * d : 2 * d + 1, :], total[2 * d + 1 : 2 * d + 2, :])

    lsend[0:1, :] = total_lanes(0)
    lsend[1:2, :] = total_lanes(1)
    l1_start, l1_wait, l1_left = exchange(NI, i, near, lambda j: lsend, rl1, near_ssem.at[1], near_rsem.at[1])
    l1_start()
    rl1[i] = lsend[...]

    columns = jnp.concatenate(
        [within_row, jnp.exp(total - within_row) * size_row, jnp.exp(within_row), jnp.zeros((104, 128), F32)],
        axis=0,
    ).T

    def head_columns(columns, base, d):
        at = base + 2 * d
        return jnp.where(low_lanes, columns[:, at : at + 1], columns[:, at + 1 : at + 2])

    mixed = conv(u, before, after)
    values = mixed[:, :128]
    writes = mixed[:, 128:192].astype(BF16)
    reads = mixed[:, 192:256].astype(BF16)

    def state_of(writes, weighted):
        return lax.dot_general(
            writes.astype(BF16),
            weighted.astype(BF16),
            (((0,), (0,)), ((), ())),
            preferred_element_type=F32,
        )

    for d in range(2):
        sp[8 * d : 8 * d + 8] = state_of(writes, values * head_columns(columns, 8, d)).astype(BF16).reshape(8, 8, 128)
    s1_start, s1_wait, s1_left = exchange(NI, i, near, lambda j: sp.at[j], rs1, near_ssem.at[2], near_rsem.at[2])
    s1_start()
    rs1[i] = sp[i]

    scores = lax.dot_general(reads, writes, (((1,), (1,)), ((), ())), preferred_element_type=F32)
    inner = []
    for h in range(2):
        fading = jnp.zeros((128, 128), F32)
        for d in range(2):
            k = 2 * d + h
            gap = columns[:, k : k + 1] - within_row[k : k + 1, :]
            mask = (ri >= ci) if d == 0 else (ri <= ci)
            fading = fading + jnp.exp(jnp.where(mask, gap, -1e30)) * size_row[k : k + 1, :]
        inner.append(dot_bf16(scores * fading, values[:, 64 * h : 64 * h + 64]))
    skips = jnp.where(low_lanes, own(skip[...], 0), own(skip[...], 1))
    local = skips * values + jnp.concatenate(inner, axis=1)
    gates = silu(gate_linear)

    l1_wait()
    l2send[...] = jnp.sum(rl1[...], axis=0)
    l2_start, l2_wait, l2_left = exchange(NA, a, far, lambda j: l2send, rl2, far_ssem.at[0], far_rsem.at[0])
    l2_start()
    rl2[a] = l2send[...]

    s1_wait()

    def fold(k, carry):
        state, product = carry
        j = k + direction * (NI - 1 - 2 * k)
        cpre[j] = state
        ppre[j] = product
        logs = rl1[j]
        factor = jnp.exp(jnp.where(direction == 0, logs[0:1, :], logs[1:2, :]))
        return factor * state + rs1[j].astype(F32), factor * product

    block_state, _ = lax.fori_loop(
        0, NI, fold, (jnp.zeros((8, 128), F32), jnp.ones((1, 128), F32))
    )
    bt[...] = block_state.astype(BF16)
    s2_start, s2_wait, s2_left = exchange(NA, a, far, lambda j: bt, rs2, far_ssem.at[1], far_rsem.at[1])
    s2_start()
    rs2[a] = bt[...]

    shift1, scale1 = vector(1, 0), 1.0 + vector(1, 1)

    def context_chunk(k, carry):
        def mod(m, carry):
            at = pl.ds(pl.multiple_of(k * 128 + m * 16, 16), 16)
            hctx[pl.ds(pl.multiple_of(m * 16, 16), 16), :] = (cn[at, :] * scale1 + shift1).astype(BF16)
            return carry

        lax.fori_loop(0, 8, mod, 0)
        found = jnp.dot(hctx[...], wall[:, 128:512], preferred_element_type=F32)
        uctx[pl.ds(pl.multiple_of(k * 128, 128), 128), :] = found.astype(BF16).astype(F32)
        return carry

    lax.fori_loop(0, CTX // 128, context_chunk, 0)
    context_mixed = conv(uctx[:, :256], jnp.zeros((1, 256), F32), jnp.zeros((1, 256), F32))
    context_values = context_mixed[:, :128]
    context_writes = context_mixed[:, 128:192]
    chunks = CTX // 128
    c_size = [own_steps(uctx[128 * c : 128 * c + 128, 256:384]) for c in range(chunks)]
    c_decay = [-size * rates for size in c_size]
    c_total = [jnp.sum(decay, axis=1, keepdims=True) for decay in c_decay]
    later = jnp.where(ri > ci, 1.0, 0.0)
    earlier = jnp.where(ri < ci, 1.0, 0.0)
    context_state = [jnp.zeros((64, 128), F32), jnp.zeros((64, 128), F32)]
    for c in range(chunks):
        after_it = sum(c_total[c + 1 :], jnp.zeros((8, 1), F32))
        before_it = sum(c_total[:c], jnp.zeros((8, 1), F32))
        rest = jnp.where(
            k8 < 2, dot_f32(c_decay[c], later) + after_it, dot_f32(c_decay[c], earlier) + before_it
        )
        turned = jnp.concatenate([jnp.exp(rest) * c_size[c], jnp.zeros((120, 128), F32)], axis=0).T
        at = slice(128 * c, 128 * c + 128)
        for d in range(2):
            context_state[d] = context_state[d] + state_of(
                context_writes[at], context_values[at] * head_columns(turned, 0, d)
            )
    for d in range(2):
        cst[8 * d : 8 * d + 8] = context_state[d].reshape(8, 8, 128)

    for left in (m1_left, relay_left, m3_left, x_left, l1_left, s1_left, l2_left, s2_left):
        left()
    up.wait_send()
    down.wait_send()
    l2_wait()
    s2_wait()
    place = a + direction * (NA - 1 - 2 * a)

    def enter(k, state):
        j = k + direction * (NA - 1 - 2 * k)
        logs = rl2[j]
        factor = jnp.exp(jnp.where(direction == 0, logs[0:1, :], logs[1:2, :]))
        return jnp.where(k < place, factor * state + rs2[j].astype(F32), state)

    entering = lax.fori_loop(0, NA, enter, cst[i])

    def hand_out(k, carry):
        osend[k] = (cpre[k] + ppre[k] * entering).astype(BF16)
        return carry

    lax.fori_loop(0, NI, hand_out, 0)
    s3_start, s3_wait, s3_left = exchange(NI, i, near, lambda j: osend.at[j], rs3, near_ssem.at[3], near_rsem.at[3])
    s3_start()
    rs3[i] = osend[i]
    s3_wait()

    mixer = local
    for d in range(2):
        came = rs3[8 * d : 8 * d + 8].reshape(64, 128)
        mixer = mixer + dot_bf16(reads, came) * head_columns(columns, 16, d)
    gated = mixer * gates
    gated = gated * lax.rsqrt(jnp.mean(gated * gated, axis=-1, keepdims=True) + EPSILON) * ggain[...]
    gated = gated.astype(BF16)
    loads[6].wait()
    for n in range(4):
        at = slice(512 * n, 512 * n + 512)
        oo[:, :, at] = (
            jnp.dot(gated, outw_v[:, at], preferred_element_type=F32).astype(BF16).reshape(NT, ROWS, 512)
        )
    o_start, o_wait, o_left = exchange(NT, t, along_tp, lambda j: oo.at[j], ro, tp_ssem.at[1], tp_rsem.at[1])
    o_start()
    ro[t] = oo[t]
    gate0 = vector(0, 2)
    o_wait()
    summed = ro[0].astype(F32)
    for j in range(1, NT):
        summed = summed + ro[j].astype(F32)
    normed_out = (
        summed * lax.rsqrt(jnp.mean(summed * summed, axis=-1, keepdims=True) + EPSILON) * pgain[...]
    )
    out[...] = (latent[...].astype(F32) + gate0 * normed_out).astype(BF16)

    s3_left()
    o_left()


def body(
    latent,
    context,
    condition,
    context_condition,
    modulation_weight,
    norm_gain,
    gate_weight,
    value_weight,
    write_weight,
    read_weight,
    step_weight,
    value_taps,
    map_taps,
    decay_rate,
    decay_jump,
    skip_gain,
    group_gain,
    output_weight,
    post_gain,
):
    vmem = pl.BlockSpec(memory_space=pltpu.VMEM)
    hbm = pl.BlockSpec(memory_space=pl.ANY)
    dma = pltpu.SemaphoreType.DMA
    return pl.pallas_call(
        kernel,
        out_shape=pltpu.VMEM((ROWS, D), BF16),
        in_specs=[hbm] * 19,
        out_specs=vmem,
        scratch_shapes=[
            pltpu.VMEM((ROWS, D), BF16),
            pltpu.VMEM((16, 128), F32),
            pltpu.VMEM((16, 128), F32),
            pltpu.VMEM((3, ROWS, 256), BF16),
            pltpu.VMEM((1, D), F32),
            pltpu.VMEM((3, 128), BF16),
            pltpu.VMEM((3, 2, 64), BF16),
            pltpu.VMEM((2, 16), F32),
            pltpu.VMEM((2, 2, 128), F32),
            pltpu.VMEM((1, 16), F32),
            pltpu.VMEM((1, 128), F32),
            pltpu.VMEM((1, D), F32),
            pltpu.VMEM((CTX, D), BF16),
            pltpu.VMEM((256, D), BF16),
            pltpu.VMEM((128, D), BF16),
            pltpu.VMEM((D, 512), BF16),
            pltpu.VMEM((NY, 4, 128), F32),
            pltpu.VMEM((NI, 4, 128), F32),
            pltpu.VMEM((NA, 4, 128), F32),
            pltpu.VMEM((4, 128), F32),
            pltpu.VMEM((NY * NT, 4, 128), F32),
            pltpu.VMEM((NT, ROWS, D), BF16),
            pltpu.VMEM((2, 1, D), F32),
            pltpu.VMEM((2, 1, D), F32),
            pltpu.VMEM((NT + 1, ROWS, D), F32),
            pltpu.VMEM((CTX, D), F32),
            pltpu.VMEM(((NT + 1) * ROWS, D), BF16),
            pltpu.VMEM((128, D), BF16),
            pltpu.VMEM((CTX, 384), F32),
            pltpu.VMEM((2, 128), F32),
            pltpu.VMEM((NI, 2, 128), F32),
            pltpu.VMEM((2, 128), F32),
            pltpu.VMEM((NA, 2, 128), F32),
            pltpu.VMEM((NI, 8, 128), BF16),
            pltpu.VMEM((NI, 8, 128), BF16),
            pltpu.VMEM((8, 128), BF16),
            pltpu.VMEM((NA, 8, 128), BF16),
            pltpu.VMEM((NI, 8, 128), F32),
            pltpu.VMEM((NI, 1, 128), F32),
            pltpu.VMEM((NI, 8, 128), F32),
            pltpu.VMEM((NI, 8, 128), BF16),
            pltpu.VMEM((NI, 8, 128), BF16),
            pltpu.VMEM((NT, ROWS, D), BF16),
            pltpu.VMEM((NT, ROWS, D), BF16),
            dma((12,)),
            dma((7,)),
            dma((4,)),
            dma((4,)),
            dma((2,)),
            dma((2,)),
            dma((2,)),
            dma((2,)),
            dma((1,)),
            dma((1,)),
            dma((NA - 1,)),
            dma((NA - 1,)),
            dma((2,)),
            dma((2,)),
        ],
        compiler_params=pltpu.CompilerParams(
            collective_id=0, has_side_effects=True, vmem_limit_bytes=60 * 1024 * 1024
        ),
    )(
        latent,
        condition.reshape(16, 128),
        context_condition.reshape(16, 128),
        modulation_weight.transpose(1, 0, 2),
        norm_gain.reshape(1, D),
        value_taps,
        map_taps,
        decay_rate,
        decay_jump,
        skip_gain.reshape(1, 16),
        group_gain.reshape(1, 128),
        post_gain.reshape(1, D),
        context,
        gate_weight,
        value_weight,
        write_weight.T,
        read_weight.T,
        step_weight.transpose(1, 2, 0).reshape(32, D),
        output_weight,
    )


def solution(mesh):
    torus = Mesh(mesh.devices.reshape(NA, NB, NY, NT), SP_TP)
    return jax.shard_map(
        body,
        mesh=torus,
        in_specs=(
            P(SP_TP, None),
            P(),
            P(),
            P(),
            P(SP, None, "tp"),
            P(),
            P(None, "tp"),
            P(None, "tp"),
            P(None, "tp"),
            P(None, "tp"),
            P(),
            P(None, "tp"),
            P(None, None, "tp"),
            P(),
            P(None, "tp", SP),
            P(),
            P("tp"),
            P("tp", None),
            P(),
        ),
        out_specs=P(SP_TP, None),
        check_vma=False,
    )
```
